128 devices in a mesh: ep: 16 (over z, x), tp: 8 (over y, core).
Axes of the slice: x: 4, y: 4, z: 4, core: 2. Of those that a mesh axis runs over, the one named last changes fastest.
Arguments:
- tokens: bfloat16 [16384, 2048], P(('ep', 'tp')), may hold values from -6 to 6
- expert_ids: int32 [16384, 4], P('ep'), may hold values from 0 to 15, all different within a row; in each aligned block of 128 rows (0 to 127, 128 to 255, ...) at most 64 rows name the same one
- gate_values: float32 [16384, 4], P('ep'), may hold values from 0.1 to 1
- norm_gain: float32 [2048], replicated, may hold values from 0.1 to 1.9
- gate_weight: bfloat16 [16, 2048, 1024], P('ep', None, 'tp'), may hold values from -0.125 to 0.125
- up_weight: bfloat16 [16, 2048, 1024], P('ep', None, 'tp'), may hold values from -0.125 to 0.125
- down_weight: bfloat16 [16, 1024, 2048], P('ep', 'tp'), may hold values from -0.1875 to 0.1875
- out_gain: float32 [2048], P('tp'), may hold values from 0.1 to 1.9
Outputs:
- mixed: bfloat16 [16384, 2048], P('ep', 'tp')
The draws below stay inside these ranges and needn't reach their ends.
Inputs may be any that keep to these rules, and one draw needn't show every extreme that they name: `expert_ids`: each row names 4 different experts of 0 to 15; within the rows of one device (aligned blocks of 128 rows) no expert is named more than 64 times, and in some blocks one expert is named exactly 64 times.
All inputs are finite; a program needn't handle non-finite values.
Results may differ from the reference program's by a relative error of at most 0.0025.
Values may be sent and summed in bfloat16 or wider, within the bound.
No kernel may reach another device: no remote copies, remote signals or barrier semaphores. Data moves between devices by JAX's collectives and lax.ppermute only.
A program may use at most 64 MiB of HBM per device.

```python
import math
import jax
import jax.numpy as jnp
import numpy as np
from jax import lax

D = 2048
FF = 1024
TOP = 4
TOK_DEV = 128
CAP = 64
EXPERTS = 16
TOKENS = 16384
N_EP = 16
N_TP = 8


def level_of(rng, extent, split, least, largest):
    factor_of = 1.0
    for dim, parts in split:
        heights = jax.random.uniform(jax.random.fold_in(jax.random.fold_in(rng, 6), dim), (parts,), jnp.float32, least / len(split), largest / len(split))
        factor_of = factor_of * jnp.repeat(jnp.exp(heights), extent[dim] // parts).reshape((-1,) + (1,) * (len(extent) - 1 - dim))
    return factor_of


def routed_block(own_key, own, number, rows, count, top, limit, lean):
    order = jax.random.permutation(own_key, count)
    heavy_load, usual = load_shares(count, rows * top, limit, lean, True), load_shares(count, rows * top, limit, lean, False)
    places = jnp.arange(count)

    def named(tallies, rotation):
        used = int((tallies > 0).sum())
        fixed = max(1, used // 4)
        shifted = fixed + (places - fixed + rotation * (used - fixed)) % max(1, count - fixed)
        return jnp.zeros((count,), jnp.int32).at[order[jnp.where(places < fixed, places, shifted)]].set(jnp.asarray(tallies, jnp.int32))

    tallies = jnp.where(number % 4 == 0, named(heavy_load, number // 4), named(usual, number - number // 4 - 1))
    mixed = jax.random.permutation(jax.random.fold_in(own, 3), count)
    source_of, sink = mixed[0:count // 2 * 2:2], mixed[1:count // 2 * 2:2]
    slack = jnp.minimum(tallies[source_of] - 1, limit - tallies[sink]) // 2
    slack = jnp.where((source_of == order[0]) | (sink == order[0]) | (tallies[sink] == 0), 0, jnp.maximum(slack, 0))
    shifted = jax.random.randint(jax.random.fold_in(own, 4), (count // 2,), 0, 1 << 20) % (slack + 1)
    tallies = tallies.at[source_of].add(-shifted).at[sink].add(shifted)
    items = jnp.searchsorted(jnp.cumsum(tallies), jnp.arange(rows * top), side="right").astype(jnp.int32)
    table = items.reshape(top, rows).T
    table = table[jax.random.permutation(jax.random.fold_in(own, 1), rows)]
    rotation = jax.random.randint(jax.random.fold_in(own, 2), (rows, 1), 0, top)
    return jnp.take_along_axis(table, (jnp.arange(top)[None, :] + rotation) % top, axis=1)


def load_shares(number_of, total, limit, lean, full):
    portions = [(1 << 20) // math.isqrt(standing ** lean) + 1 for standing in range(1, number_of + 1)]
    largest = limit if full else min(limit, max(-(-total // number_of), total * portions[0] // sum(portions)))
    least = 1 if total - largest >= number_of - 1 else 0
    given, surplus = [largest] + [least] * (number_of - 1), total - largest - least * (number_of - 1)
    while surplus > 0:
        candidates = [i for i in range(1, number_of) if given[i] < largest] or [i for i in range(1, number_of) if given[i] < limit]
        mass, left = sum([portions[i] for i in candidates]), surplus
        for i in candidates:
            addition = min(limit - given[i], max(1, left * portions[i] // mass), surplus)
            given[i] = given[i] + addition
            surplus = surplus - addition
    return np.array(given)


def centred(key, dims, width, bound, pieces=(), held_as=jnp.bfloat16):
    values = width * jax.random.normal(key, dims, jnp.float32)
    if pieces:
        values = values * level_of(key, dims, pieces, -0.22, 0.18)
    return jnp.clip(values, -bound, bound).astype(held_as)


def setup_inputs(seed: int = 0) -> dict:
    key_of = jax.random.split(jax.random.key(seed), 9)
    tokens = centred(key_of[0], (TOKENS, D), 1.0, 6.0, ((0, 128),))
    expert_ids_keys = jax.random.split(jax.random.fold_in(key_of[1], 1), TOKENS // TOK_DEV)
    expert_ids_turns = jax.random.permutation(jax.random.fold_in(key_of[1], 3), TOKENS // TOK_DEV)
    expert_ids = jax.vmap(lambda own, number: routed_block(jax.random.fold_in(key_of[1], 2), own, number, TOK_DEV, EXPERTS, TOP, CAP, 2))(expert_ids_keys, expert_ids_turns).reshape((TOKENS, TOP))
    gate_values = jnp.clip(0.1 + 0.9 * jax.random.uniform(key_of[2], (TOKENS, TOP), jnp.float32) ** level_of(key_of[2], (TOKENS, TOP), ((0, 16),), -0.2, 0.2), 0.1, 1.0)
    norm_gain = jnp.clip(1.0 + 0.18 * jax.random.normal(key_of[3], (D,), jnp.float32), 0.1, 1.9)
    gate_weight = centred(key_of[4], (EXPERTS, D, FF), D ** -0.5, 0.125, ((0, 16), (2, 8)))
    up_weight = centred(key_of[5], (EXPERTS, D, FF), D ** -0.5, 0.125, ((0, 16), (2, 8)))
    down_weight = centred(key_of[6], (EXPERTS, FF, D), FF ** -0.5, 0.1875, ((0, 16), (1, 8)))
    out_gain = jnp.clip(1.0 + 0.18 * jax.random.normal(key_of[7], (D,), jnp.float32), 0.1, 1.9)
    return dict(tokens=tokens, expert_ids=expert_ids, gate_values=gate_values, norm_gain=norm_gain, gate_weight=gate_weight, up_weight=up_weight, down_weight=down_weight, out_gain=out_gain)


epsilon = 1e-05
clamp_limit = 7.0
sigmoid_alpha = 1.702

def rms_rows(values, gain):
    mean_sq = lax.optimization_barrier(jnp.mean(values * values, axis=-1, keepdims=True))
    return values * lax.rsqrt(mean_sq + epsilon) * gain

def clamped_unit(gate_part, up_part):
    glu_part = jnp.minimum(gate_part, clamp_limit)
    lin_part = jnp.clip(up_part, -clamp_limit, clamp_limit)
    return glu_part * jax.nn.sigmoid(sigmoid_alpha * glu_part) * (lin_part + 1.0)

def reference(tokens, expert_ids, gate_values, norm_gain, gate_weight, up_weight, down_weight, out_gain):
    normed = rms_rows(tokens.astype(jnp.float32), norm_gain).astype(jnp.bfloat16)
    blocks = expert_ids.reshape(N_EP * N_TP, TOK_DEV * TOP)
    onehot = (blocks[:, :, None] == jnp.arange(EXPERTS, dtype=jnp.int32)[None, None, :]).astype(jnp.int32)
    slot_num = lax.optimization_barrier(jnp.sum((jnp.cumsum(onehot, axis=1) - onehot) * onehot, axis=2)).reshape(TOKENS, TOP)
    source = (jnp.arange(TOKENS, dtype=jnp.int32) // TOK_DEV)[:, None]
    position = (source * CAP + slot_num).astype(jnp.int32)
    table_rows = N_EP * N_TP * CAP
    token_index = jnp.broadcast_to(jnp.arange(TOKENS, dtype=jnp.int32)[:, None], (TOKENS, TOP)).reshape(-1)
    padded = jnp.concatenate([normed, jnp.zeros((1, D), jnp.bfloat16)], axis=0)

    def one_expert(running, inputs):
        expert, w_gate, w_up, w_down = inputs
        chosen = expert_ids == expert
        where_row = jnp.where(chosen, position, table_rows).astype(jnp.int32)
        owner_row = jnp.full((table_rows + 1,), TOKENS, jnp.int32).at[where_row.reshape(-1)].set(token_index)
        rows_in = padded[owner_row[:table_rows]].astype(jnp.float32)
        gate_part = jnp.dot(rows_in, w_gate.astype(jnp.float32), precision=lax.Precision.HIGHEST)
        up_part = jnp.dot(rows_in, w_up.astype(jnp.float32), precision=lax.Precision.HIGHEST)
        activated = clamped_unit(gate_part, up_part).astype(jnp.bfloat16)
        activated = lax.optimization_barrier(activated).astype(jnp.float32)
        outputs = jnp.dot(activated, w_down.astype(jnp.float32), precision=lax.Precision.HIGHEST).astype(jnp.bfloat16)
        outputs = lax.optimization_barrier(outputs).astype(jnp.float32)
        outputs = jnp.concatenate([outputs, jnp.zeros((1, D), jnp.float32)], axis=0)
        for choice_k in range(TOP):
            weight = jnp.where(chosen[:, choice_k], gate_values[:, choice_k], jnp.float32(0.0))
            running = running + weight[:, None] * outputs[where_row[:, choice_k]]
        return (running, None)
    combined, _ = lax.scan(one_expert, jnp.zeros((TOKENS, D), jnp.float32), (jnp.arange(EXPERTS, dtype=jnp.int32), gate_weight, up_weight, down_weight))
    mean_sq = lax.optimization_barrier(jnp.mean(combined * combined, axis=1, keepdims=True))
    return (combined * lax.rsqrt(mean_sq + epsilon) * out_gain).astype(jnp.bfloat16)
```

```python
import functools
import jax
import jax.numpy as jnp
from jax import lax
from jax.experimental import pallas as pl
from jax.experimental.pallas import tpu as pltpu
from jax.sharding import PartitionSpec as P

epsilon = 1e-05
clamp_limit = 7.0
sigmoid_alpha = 1.702
f32, bf16 = jnp.float32, jnp.bfloat16


def routing(ids, experts):
    tokens, top = ids.shape
    lane = lax.broadcasted_iota(jnp.int32, (tokens, experts), 1)
    named = jnp.zeros((tokens, experts), f32)
    for k in range(top):
        named = named + jnp.where(ids[:, k : k + 1] == lane, 1.0, 0.0)
    row = lax.broadcasted_iota(jnp.int32, (tokens, tokens), 0)
    col = lax.broadcasted_iota(jnp.int32, (tokens, tokens), 1)
    below = jnp.where(col < row, 1.0, 0.0).astype(bf16)
    earlier = jnp.dot(below, named.astype(bf16), preferred_element_type=f32)
    return named, earlier


def dispatch_kernel(rank, tokens_ref, ids_ref, gain_ref, out_ref, normed_ref, slot_ref, *, experts, cap):
    e = pl.program_id(0)
    tokens = tokens_ref.shape[0]

    @pl.when(e == 0)
    def _():
        values = tokens_ref[...].astype(f32)
        mean_sq = jnp.mean(values * values, axis=-1, keepdims=True)
        normed_ref[...] = (values * lax.rsqrt(mean_sq + epsilon) * gain_ref[...]).astype(bf16)
        named, earlier = routing(ids_ref[...], experts)
        slots = jnp.where(named > 0.5, earlier, -1.0)
        padded = jnp.concatenate([slots, jnp.full((tokens, tokens - experts), -1.0, f32)], axis=1)
        slot_ref[...] = jnp.transpose(padded)[:experts, :]

    slot_of = slot_ref[pl.ds(e, 1), :]
    want = lax.broadcasted_iota(jnp.int32, (cap, tokens), 0).astype(f32)
    chosen = jnp.where(slot_of == want, 1.0, 0.0).astype(bf16)
    out_ref[0] = jnp.dot(chosen, normed_ref[...], preferred_element_type=f32).astype(bf16)


def dispatch(rank, tokens, ids, gain, experts, cap):
    rows, width = tokens.shape
    return pl.pallas_call(
        functools.partial(dispatch_kernel, experts=experts, cap=cap),
        out_shape=jax.ShapeDtypeStruct((experts, cap, width), bf16),
        grid_spec=pltpu.PrefetchScalarGridSpec(
            num_scalar_prefetch=1,
            grid=(experts,),
            in_specs=[
                pl.BlockSpec((rows, width), lambda e, r: (0, 0)),
                pl.BlockSpec((rows, ids.shape[1]), lambda e, r: (r[0], 0)),
                pl.BlockSpec((1, width), lambda e, r: (0, 0)),
            ],
            out_specs=pl.BlockSpec((1, cap, width), lambda e, r: (e, 0, 0)),
            scratch_shapes=[pltpu.VMEM((rows, width), bf16), pltpu.VMEM((experts, rows), f32)],
        ),
        name="dispatch",
    )(rank, tokens, ids, gain)


def expert_kernel(rows_hbm, *rest, parts):
    gu = rest[:parts]
    dn = rest[parts : 2 * parts]
    out_hbm = rest[2 * parts]
    rows_v, gu_v, dn_v, act_v, out_v, row_sem, gu_sem, dn_sem, out_sem = rest[2 * parts + 1 :]
    hid = dn[0].shape[0]
    total, width = rows_v.shape
    nrow = row_sem.shape[0]
    step = total // nrow
    nout = out_sem.shape[0]
    ocols = width // nout
    row_copies = [
        pltpu.make_async_copy(
            rows_hbm.at[pl.ds(i * step, step)], rows_v.at[pl.ds(i * step, step)], row_sem.at[i]
        )
        for i in range(nrow)
    ]
    gu_copies = [pltpu.make_async_copy(gu[i], gu_v.at[i], gu_sem.at[i]) for i in range(parts)]
    dn_copies = [
        pltpu.make_async_copy(dn[i], dn_v.at[pl.ds(i * hid, hid)], dn_sem.at[i]) for i in range(parts)
    ]
    gu_copies[0].start()
    for c in row_copies + gu_copies[1:] + dn_copies:
        c.start()
    for i in range(parts):
        gu_copies[i].wait()
        for m in range(nrow):
            if i == 0:
                row_copies[m].wait()
            span = pl.ds(m * step, step)
            h = jnp.dot(rows_v[span, :], gu_v[i], preferred_element_type=f32)
            g = jnp.minimum(h[:, :hid], clamp_limit)
            u = jnp.clip(h[:, hid:], -clamp_limit, clamp_limit)
            act = g * jax.nn.sigmoid(sigmoid_alpha * g) * (u + 1.0)
            act_v[span, i * hid : (i + 1) * hid] = act.astype(bf16)
    for c in dn_copies:
        c.wait()
    out_copies = []
    for n in range(nout):
        cols = pl.ds(n * ocols, ocols)
        out_v[:, cols] = jnp.dot(act_v[...], dn_v[:, cols], preferred_element_type=f32).astype(bf16)
        c = pltpu.make_async_copy(out_v.at[:, cols], out_hbm.at[:, cols], out_sem.at[n])
        c.start()
        out_copies.append(c)
    for c in out_copies:
        c.wait()


def expert_unit(rows, gu, dn):
    total, width = rows.shape
    parts = len(gu)
    hid = dn[0].shape[0]
    hbm = pl.BlockSpec(memory_space=pl.ANY)
    return pl.pallas_call(
        functools.partial(expert_kernel, parts=parts),
        out_shape=jax.ShapeDtypeStruct((total, width), bf16),
        in_specs=[hbm] * (1 + 2 * parts),
        out_specs=hbm,
        scratch_shapes=[
            pltpu.VMEM((total, width), bf16),
            pltpu.VMEM((parts, width, 2 * hid), bf16),
            pltpu.VMEM((parts * hid, width), bf16),
            pltpu.VMEM((total, parts * hid), bf16),
            pltpu.VMEM((total, width), bf16),
            pltpu.SemaphoreType.DMA((4,)),
            pltpu.SemaphoreType.DMA((parts,)),
            pltpu.SemaphoreType.DMA((parts,)),
            pltpu.SemaphoreType.DMA((4,)),
        ],
        compiler_params=pltpu.CompilerParams(vmem_limit_bytes=56 * 2**20),
        cost_estimate=pl.CostEstimate(
            flops=6 * total * width * parts * hid, bytes_accessed=20 * 2**20, transcendentals=total * parts * hid
        ),
        name="expert_unit",
    )(rows, *gu, *dn)


def combine_kernel(rank, ids_ref, gates_ref, gain_ref, back_ref, out_ref, acc_ref, *, experts, cap, group, slices):
    step = pl.program_id(0)
    tokens, top = ids_ref.shape

    @pl.when(step == 0)
    def _():
        acc_ref[...] = jnp.zeros_like(acc_ref)

    ids = ids_ref[...]
    gates = gates_ref[...]
    named, earlier = routing(ids, experts)
    lane = lax.broadcasted_iota(jnp.int32, (tokens, experts), 1)
    weight = jnp.zeros((tokens, experts), f32)
    for k in range(top):
        weight = weight + jnp.where(ids[:, k : k + 1] == lane, gates[:, k : k + 1], 0.0)
    place = lane.astype(f32) * cap + earlier
    pieces = []
    col = lax.broadcasted_iota(jnp.int32, (tokens, group * cap), 1).astype(f32)
    col = col + (step * (group * cap)).astype(f32)
    spread = jnp.zeros((tokens, group * cap), f32)
    for e in range(experts):
        hit = (col == place[:, e : e + 1]) & (named[:, e : e + 1] > 0.5)
        spread = jnp.where(hit, weight[:, e : e + 1], spread)
    for _ in range(3):
        part = spread.astype(bf16)
        pieces.append(part)
        spread = spread - part.astype(f32)
    stacked = jnp.concatenate(pieces, axis=0)
    prod = jnp.dot(stacked, back_ref[...], preferred_element_type=f32)
    acc_ref[...] += prod[:tokens] + prod[tokens : 2 * tokens] + prod[2 * tokens :]

    @pl.when(step == pl.num_programs(0) - 1)
    def _():
        combined = acc_ref[...]
        mean_sq = jnp.mean(combined * combined, axis=-1, keepdims=True)
        mixed = (combined * lax.rsqrt(mean_sq + epsilon) * gain_ref[...]).astype(bf16)
        w = mixed.shape[1] // slices
        for i in range(slices):
            out_ref[i] = mixed[:, i * w : (i + 1) * w]


def combine(rank, ids, gates, gain, back, rows, experts, cap, slices):
    width = back.shape[1]
    group = 4
    return pl.pallas_call(
        functools.partial(combine_kernel, experts=experts, cap=cap, group=group, slices=slices),
        out_shape=jax.ShapeDtypeStruct((slices, rows, width // slices), bf16),
        grid_spec=pltpu.PrefetchScalarGridSpec(
            num_scalar_prefetch=1,
            grid=(experts // group,),
            in_specs=[
                pl.BlockSpec((rows, ids.shape[1]), lambda s, r: (r[0], 0)),
                pl.BlockSpec((rows, ids.shape[1]), lambda s, r: (r[0], 0)),
                pl.BlockSpec((1, width), lambda s, r: (0, 0)),
                pl.BlockSpec((group * cap, width), lambda s, r: (s, 0)),
            ],
            out_specs=pl.BlockSpec((slices, rows, width // slices), lambda s, r: (0, 0, 0)),
            scratch_shapes=[pltpu.VMEM((rows, width), f32)],
        ),
        name="combine",
    )(rank, ids, gates, gain, back)


def moved(x, step):
    n = lax.axis_size("tp")
    return lax.ppermute(x, "tp", [(i, step(i)) for i in range(n)])


def local(
    tokens, expert_ids, gate_values, norm_gain, gate_weight, up_weight, down_weight, out_gain
):
    experts = lax.axis_size("ep")
    n_tp = lax.axis_size("tp")
    rows, width = tokens.shape
    cap = rows // 2
    rank = lax.axis_index("tp").reshape(1).astype(jnp.int32)

    gu_own = jnp.concatenate([gate_weight[0], up_weight[0]], axis=1)
    dn_own = down_weight[0]

    def around(x):
        out = [x]
        for d in (2, n_tp - 2, 4):
            out.append(moved(x, lambda i: (i + d) % n_tp))
        return out

    gu_near = around(gu_own)
    dn_near = around(dn_own)
    gu = gu_near + [moved(x, lambda i: i ^ 1) for x in gu_near]
    dn = dn_near + [moved(x, lambda i: i ^ 1) for x in dn_near]

    gain_full = lax.all_gather(out_gain, "tp", axis=0, tiled=True)
    outgoing = dispatch(rank, tokens, expert_ids, norm_gain.reshape(1, width), experts, cap)
    arrived = lax.all_to_all(outgoing, "ep", split_axis=0, concat_axis=0, tiled=True)
    result = expert_unit(arrived.reshape(experts * cap, width), gu, dn)
    back = lax.all_to_all(
        result.reshape(experts, cap, width), "ep", split_axis=0, concat_axis=0, tiled=True
    )
    mixed = combine(
        rank, expert_ids, gate_values, gain_full.reshape(1, width),
        back.reshape(experts * cap, width), rows, experts, cap, n_tp,
    )
    final = lax.all_to_all(mixed, "tp", split_axis=0, concat_axis=0, tiled=True)
    return final.reshape(n_tp * rows, width // n_tp)


def solution(mesh):
    in_specs = (
        P(("ep", "tp"), None),
        P("ep", None),
        P("ep", None),
        P(),
        P("ep", None, "tp"),
        P("ep", None, "tp"),
        P("ep", "tp", None),
        P("tp"),
    )
    out_specs = P("ep", "tp")
    return jax.shard_map(local, mesh=mesh, in_specs=in_specs, out_specs=out_specs, check_vma=False)
```

```python
import functools
import jax
import jax.numpy as jnp
from jax import lax
from jax.experimental import pallas as pl
from jax.experimental.pallas import tpu as pltpu
from jax.sharding import PartitionSpec as P

epsilon = 1e-05
clamp_limit = 7.0
sigmoid_alpha = 1.702
f32, bf16 = jnp.float32, jnp.bfloat16


def routing(ids, experts):
    top, tokens = ids.shape
    line = lax.broadcasted_iota(jnp.int32, (experts, tokens), 0)
    named = jnp.zeros((experts, tokens), f32)
    for k in range(top):
        named = named + jnp.where(ids[k : k + 1, :] == line, 1.0, 0.0)
    row = lax.broadcasted_iota(jnp.int32, (tokens, tokens), 0)
    col = lax.broadcasted_iota(jnp.int32, (tokens, tokens), 1)
    before = jnp.where(row < col, 1.0, 0.0).astype(bf16)
    earlier = jnp.dot(named.astype(bf16), before, preferred_element_type=f32)
    return jnp.where(named > 0.5, earlier, -1000.0)


def dispatch_kernel(rank, tokens_ref, ids_ref, gain_ref, out_ref, normed_ref, slot_ref, *, experts, cap):
    tokens = tokens_ref.shape[0]
    group = out_ref.shape[0]

    @pl.when(pl.program_id(0) == 0)
    def _():
        values = tokens_ref[...].astype(f32)
        mean_sq = jnp.mean(values * values, axis=-1, keepdims=True)
        normed_ref[...] = (values * lax.rsqrt(mean_sq + epsilon) * gain_ref[...]).astype(bf16)
        slots = routing(ids_ref[...], experts)
        for i in range(experts // group):
            slot_ref[i] = slots[i * group : (i + 1) * group]

    slots = slot_ref[pl.program_id(0)]
    want = lax.broadcasted_iota(jnp.int32, (cap, tokens), 0).astype(f32)
    chosen = jnp.concatenate(
        [jnp.where(slots[i : i + 1] == want, 1.0, 0.0).astype(bf16) for i in range(group)], axis=0
    )
    picked = jnp.dot(chosen, normed_ref[...], preferred_element_type=f32).astype(bf16)
    for i in range(group):
        out_ref[i] = picked[i * cap : (i + 1) * cap]


def dispatch(rank, tokens, ids, gain, experts, cap):
    rows, width = tokens.shape
    group = 4
    return pl.pallas_call(
        functools.partial(dispatch_kernel, experts=experts, cap=cap),
        out_shape=jax.ShapeDtypeStruct((experts, cap, width), bf16),
        grid_spec=pltpu.PrefetchScalarGridSpec(
            num_scalar_prefetch=1,
            grid=(experts // group,),
            in_specs=[
                pl.BlockSpec((rows, width), lambda e, r: (0, 0)),
                pl.BlockSpec((ids.shape[0], rows), lambda e, r: (0, r[0])),
                pl.BlockSpec((1, width), lambda e, r: (0, 0)),
            ],
            out_specs=pl.BlockSpec((group, cap, width), lambda e, r: (e, 0, 0)),
            scratch_shapes=[
                pltpu.VMEM((rows, width), bf16),
                pltpu.VMEM((experts // group, group, rows), f32),
            ],
        ),
        name="dispatch",
    )(rank, tokens, ids, gain)


def expert_kernel(rows_hbm, *rest, parts):
    gu = rest[:parts]
    dn = rest[parts : 2 * parts]
    out_hbm = rest[2 * parts]
    rows_v, gu_v, dn_v, act_v, out_v, row_sem, gu_sem, dn_sem, out_sem = rest[2 * parts + 1 :]
    hid = dn[0].shape[0]
    total, width = rows_v.shape
    nrow = row_sem.shape[0]
    step = total // nrow
    nout = out_sem.shape[0]
    ocols = width // nout
    row_copies = [
        pltpu.make_async_copy(
            rows_hbm.at[pl.ds(i * step, step)], rows_v.at[pl.ds(i * step, step)], row_sem.at[i]
        )
        for i in range(nrow)
    ]
    gu_copies = [pltpu.make_async_copy(gu[i], gu_v.at[i], gu_sem.at[i]) for i in range(parts)]
    dn_copies = [
        pltpu.make_async_copy(dn[i], dn_v.at[pl.ds(i * hid, hid)], dn_sem.at[i]) for i in range(parts)
    ]
    gu_copies[0].start()
    for c in row_copies:
        c.start()
    gu_copies[1].start()
    for i in range(parts):
        if i + 2 < parts:
            gu_copies[i + 2].start()
        dn_copies[i].start()
        gu_copies[i].wait()
        for m in range(nrow):
            if i == 0:
                row_copies[m].wait()
            span = pl.ds(m * step, step)
            h = jnp.dot(rows_v[span, :], gu_v[i], preferred_element_type=f32)
            g = jnp.minimum(h[:, :hid], clamp_limit)
            u = jnp.clip(h[:, hid:], -clamp_limit, clamp_limit)
            act = g * jax.nn.sigmoid(sigmoid_alpha * g) * (u + 1.0)
            act_v[span, i * hid : (i + 1) * hid] = act.astype(bf16)
    for c in dn_copies:
        c.wait()
    out_copies = []
    for n in range(nout):
        cols = pl.ds(n * ocols, ocols)
        out_v[:, cols] = jnp.dot(act_v[...], dn_v[:, cols], preferred_element_type=f32).astype(bf16)
        c = pltpu.make_async_copy(out_v.at[:, cols], out_hbm.at[:, cols], out_sem.at[n])
        c.start()
        out_copies.append(c)
    for c in out_copies:
        c.wait()


def expert_unit(rows, gu, dn):
    total, width = rows.shape
    parts = len(gu)
    hid = dn[0].shape[0]
    hbm = pl.BlockSpec(memory_space=pl.ANY)
    return pl.pallas_call(
        functools.partial(expert_kernel, parts=parts),
        out_shape=jax.ShapeDtypeStruct((total, width), bf16),
        in_specs=[hbm] * (1 + 2 * parts),
        out_specs=hbm,
        scratch_shapes=[
            pltpu.VMEM((total, width), bf16),
            pltpu.VMEM((parts, width, 2 * hid), bf16),
            pltpu.VMEM((parts * hid, width), bf16),
            pltpu.VMEM((total, parts * hid), bf16),
            pltpu.VMEM((total, width), bf16),
            pltpu.SemaphoreType.DMA((4,)),
            pltpu.SemaphoreType.DMA((parts,)),
            pltpu.SemaphoreType.DMA((parts,)),
            pltpu.SemaphoreType.DMA((4,)),
        ],
        compiler_params=pltpu.CompilerParams(vmem_limit_bytes=56 * 2**20),
        cost_estimate=pl.CostEstimate(
            flops=6 * total * width * parts * hid, bytes_accessed=20 * 2**20, transcendentals=total * parts * hid
        ),
        name="expert_unit",
    )(rows, *gu, *dn)


def combine_kernel(rank, ids_ref, gates_ref, gain_ref, back_hbm, out_ref, back_v, spread_v, acc_v, sem, *, experts, cap):
    top, tokens = ids_ref.shape
    width = back_v.shape[1]
    chunks = sem.shape[0]
    cols = width // chunks
    copies = [
        pltpu.make_async_copy(
            back_hbm.at[:, pl.ds(c * cols, cols)], back_v.at[:, pl.ds(c * cols, cols)], sem.at[c]
        )
        for c in range(chunks)
    ]
    for c in copies:
        c.start()
    ids = ids_ref[...]
    gates = gates_ref[...]
    line = lax.broadcasted_iota(jnp.int32, (experts, tokens), 0)
    weight = jnp.zeros((experts, tokens), f32)
    for k in range(top):
        weight = weight + jnp.where(ids[k : k + 1, :] == line, gates[k : k + 1, :], 0.0)
    filler = jnp.zeros((tokens - 2 * experts, tokens), f32)
    table = jnp.transpose(jnp.concatenate([routing(ids, experts), weight, filler], axis=0))
    col = lax.broadcasted_iota(jnp.int32, (tokens, 2 * cap), 1).astype(f32)
    for e in range(0, experts, 2):
        slot_a, slot_b = table[:, e : e + 1], table[:, e + 1 : e + 2] + cap
        gate_a, gate_b = table[:, experts + e : experts + e + 1], table[:, experts + e + 1 : experts + e + 2]
        spread = jnp.where(col == slot_a, gate_a, 0.0) + jnp.where(col == slot_b, gate_b, 0.0)
        for p in range(3):
            part = spread.astype(bf16)
            spread_v[p * tokens : (p + 1) * tokens, e * cap : (e + 2) * cap] = part
            spread = spread - part.astype(f32)
    total_sq = jnp.zeros((tokens, 1), f32)
    for c in range(chunks):
        copies[c].wait()
        span = pl.ds(c * cols, cols)
        prod = jnp.dot(spread_v[...], back_v[:, span], preferred_element_type=f32)
        combined = prod[:tokens] + prod[tokens : 2 * tokens] + prod[2 * tokens :]
        total_sq = total_sq + jnp.sum(combined * combined, axis=-1, keepdims=True)
        acc_v[:, span] = combined
    scale = lax.rsqrt(total_sq / width + epsilon)
    slices, _, w = out_ref.shape
    for i in range(slices):
        span = pl.ds(i * w, w)
        out_ref[i] = (acc_v[:, span] * scale * gain_ref[:, span]).astype(bf16)


def combine(rank, ids, gates, gain, back, rows, experts, cap, slices):
    width = back.shape[1]
    top = ids.shape[0]
    return pl.pallas_call(
        functools.partial(combine_kernel, experts=experts, cap=cap),
        out_shape=jax.ShapeDtypeStruct((slices, rows, width // slices), bf16),
        grid_spec=pltpu.PrefetchScalarGridSpec(
            num_scalar_prefetch=1,
            grid=(1,),
            in_specs=[
                pl.BlockSpec((top, rows), lambda s, r: (0, r[0])),
                pl.BlockSpec((top, rows), lambda s, r: (0, r[0])),
                pl.BlockSpec((1, width), lambda s, r: (0, 0)),
                pl.BlockSpec(memory_space=pl.ANY),
            ],
            out_specs=pl.BlockSpec((slices, rows, width // slices), lambda s, r: (0, 0, 0)),
            scratch_shapes=[
                pltpu.VMEM((experts * cap, width), bf16),
                pltpu.VMEM((3 * rows, experts * cap), bf16),
                pltpu.VMEM((rows, width), f32),
                pltpu.SemaphoreType.DMA((4,)),
            ],
        ),
        name="combine",
    )(rank, ids, gates, gain, back)


def moved(x, step):
    n = lax.axis_size("tp")
    return lax.ppermute(x, "tp", [(i, step(i)) for i in range(n)])


def local(
    tokens, expert_ids, gate_values, norm_gain, gate_weight, up_weight, down_weight, out_gain
):
    experts = lax.axis_size("ep")
    n_tp = lax.axis_size("tp")
    rows, width = tokens.shape
    cap = rows // 2
    rank = lax.axis_index("tp").reshape(1).astype(jnp.int32)
    ids, gates = expert_ids.T, gate_values.T

    gu_own = jnp.concatenate([gate_weight[0], up_weight[0]], axis=1)
    dn_own = down_weight[0]

    def around(x):
        out = [x]
        for d in (2, n_tp - 2, 4):
            out.append(moved(x, lambda i: (i + d) % n_tp))
        return out

    def across(xs):
        out = []
        for x in xs:
            out.append(moved(x, lambda i: i ^ 1))
        return out

    gu_near = around(gu_own)
    dn_near = around(dn_own)
    gu = gu_near + across(gu_near)
    dn = dn_near + across(dn_near)

    gain_full = lax.all_gather(out_gain, "tp", axis=0, tiled=True)
    outgoing = dispatch(rank, tokens, ids, norm_gain.reshape(1, width), experts, cap)
    arrived = lax.all_to_all(outgoing, "ep", split_axis=0, concat_axis=0, tiled=True)
    result = expert_unit(arrived.reshape(experts * cap, width), gu, dn)
    back = lax.all_to_all(
        result.reshape(experts, cap, width), "ep", split_axis=0, concat_axis=0, tiled=True
    )
    mixed = combine(
        rank, ids, gates, gain_full.reshape(1, width),
        back.reshape(experts * cap, width), rows, experts, cap, n_tp,
    )
    final = lax.all_to_all(mixed, "tp", split_axis=0, concat_axis=0, tiled=True)
    return final.reshape(n_tp * rows, width // n_tp)


def solution(mesh):
    in_specs = (
        P(("ep", "tp"), None),
        P("ep", None),
        P("ep", None),
        P(),
        P("ep", None, "tp"),
        P("ep", None, "tp"),
        P("ep", "tp", None),
        P("tp"),
    )
    out_specs = P("ep", "tp")
    return jax.shard_map(local, mesh=mesh, in_specs=in_specs, out_specs=out_specs, check_vma=False)
```

```python
import functools
import jax
import jax.numpy as jnp
from jax import lax
from jax.experimental import pallas as pl
from jax.experimental.pallas import tpu as pltpu
from jax.sharding import PartitionSpec as P

epsilon = 1e-05
clamp_limit = 7.0
sigmoid_alpha = 1.702
f32, bf16 = jnp.float32, jnp.bfloat16


def SPLIT(cap):
    return (cap,)


def routing(ids, experts):
    top, tokens = ids.shape
    line = lax.broadcasted_iota(jnp.int32, (experts, tokens), 0)
    named = jnp.zeros((experts, tokens), f32)
    for k in range(top):
        named = named + jnp.where(ids[k : k + 1, :] == line, 1.0, 0.0)
    row = lax.broadcasted_iota(jnp.int32, (tokens, tokens), 0)
    col = lax.broadcasted_iota(jnp.int32, (tokens, tokens), 1)
    before = jnp.where(row < col, 1.0, 0.0).astype(bf16)
    earlier = jnp.dot(named.astype(bf16), before, preferred_element_type=f32)
    return jnp.where(named > 0.5, earlier, -1000.0)


def dispatch_kernel(rank, tokens_ref, ids_ref, gain_ref, *rest, experts, cap):
    outs, (normed_ref, slot_ref) = rest[:-2], rest[-2:]
    tokens = tokens_ref.shape[0]
    group = outs[0].shape[0]

    @pl.when(pl.program_id(0) == 0)
    def _():
        values = tokens_ref[...].astype(f32)
        mean_sq = jnp.mean(values * values, axis=-1, keepdims=True)
        normed_ref[...] = (values * lax.rsqrt(mean_sq + epsilon) * gain_ref[...]).astype(bf16)
        slots = routing(ids_ref[...], experts)
        for i in range(experts // group):
            slot_ref[i] = slots[i * group : (i + 1) * group]

    slots = slot_ref[pl.program_id(0)]
    want = lax.broadcasted_iota(jnp.int32, (cap, tokens), 0).astype(f32)
    chosen = jnp.concatenate(
        [jnp.where(slots[i : i + 1] == want, 1.0, 0.0).astype(bf16) for i in range(group)], axis=0
    )
    picked = jnp.dot(chosen, normed_ref[...], preferred_element_type=f32).astype(bf16)
    for i in range(group):
        at = i * cap
        for out in outs:
            out[i] = picked[at : at + out.shape[1]]
            at += out.shape[1]


def dispatch(rank, tokens, ids, gain, experts, split):
    rows, width = tokens.shape
    group = 4
    return pl.pallas_call(
        functools.partial(dispatch_kernel, experts=experts, cap=sum(split)),
        out_shape=[jax.ShapeDtypeStruct((experts, n, width), bf16) for n in split],
        grid_spec=pltpu.PrefetchScalarGridSpec(
            num_scalar_prefetch=1,
            grid=(experts // group,),
            in_specs=[
                pl.BlockSpec((rows, width), lambda e, r: (0, 0)),
                pl.BlockSpec((ids.shape[0], rows), lambda e, r: (0, r[0])),
                pl.BlockSpec((1, width), lambda e, r: (0, 0)),
            ],
            out_specs=[pl.BlockSpec((group, n, width), lambda e, r: (e, 0, 0)) for n in split],
            scratch_shapes=[
                pltpu.VMEM((rows, width), bf16),
                pltpu.VMEM((experts // group, group, rows), f32),
            ],
        ),
        name="dispatch",
    )(rank, tokens, ids, gain)


def expert_kernel(rows_hbm, *rest, gu_parts, dn_parts):
    gu = rest[: len(gu_parts)]
    dn = rest[len(gu_parts) : len(gu_parts) + len(dn_parts)]
    out_hbm, rows_v, gu_v, dn_v, act_v, out_v, row_sem, gu_sem, dn_sem, out_sem = rest[len(gu_parts) + len(dn_parts) :]
    parts = gu_v.shape[0]
    hid = gu_v.shape[2] // 2
    total, width = rows_v.shape
    nrow = row_sem.shape[0]
    step = total // nrow
    nout = out_sem.shape[0]
    ocols = width // nout

    row_copies = [
        pltpu.make_async_copy(
            rows_hbm.at[pl.ds(i * step, step)], rows_v.at[pl.ds(i * step, step)], row_sem.at[i]
        )
        for i in range(nrow)
    ]
    gu_copies = [[] for _ in range(parts)]
    for j, (i, at, size) in enumerate(gu_parts):
        gu_copies[i].append(
            pltpu.make_async_copy(gu[j], gu_v.at[i, pl.ds(at, size)], gu_sem.at[j])
        )
    dn_copies = [[] for _ in range(parts)]
    for j, (i, at, size) in enumerate(dn_parts):
        dn_copies[i].append(
            pltpu.make_async_copy(dn[j], dn_v.at[pl.ds(i * hid + at, size)], dn_sem.at[j])
        )
    for c in gu_copies[0] + row_copies + gu_copies[1]:
        c.start()
    for i in range(parts):
        for c in (gu_copies[i + 2] if i + 2 < parts else []) + dn_copies[i]:
            c.start()
        for c in gu_copies[i]:
            c.wait()
        for m in range(nrow):
            if i == 0:
                row_copies[m].wait()
            span = pl.ds(m * step, step)
            h = jnp.dot(rows_v[span, :], gu_v[i], preferred_element_type=f32)
            g = jnp.minimum(h[:, :hid], clamp_limit)
            u = jnp.clip(h[:, hid:], -clamp_limit, clamp_limit)
            act = g * jax.nn.sigmoid(sigmoid_alpha * g) * (u + 1.0)
            act_v[span, i * hid : (i + 1) * hid] = act.astype(bf16)
    for cs in dn_copies:
        for c in cs:
            c.wait()
    out_copies = []
    for n in range(nout):
        cols = pl.ds(n * ocols, ocols)
        out_v[:, cols] = jnp.dot(act_v[...], dn_v[:, cols], preferred_element_type=f32).astype(bf16)
        c = pltpu.make_async_copy(out_v.at[:, cols], out_hbm.at[:, cols], out_sem.at[n])
        c.start()
        out_copies.append(c)
    for c in out_copies:
        c.wait()


def expert_unit(rows, gu, dn, parts, hid):
    total, width = rows.shape
    hbm = pl.BlockSpec(memory_space=pl.ANY)
    return pl.pallas_call(
        functools.partial(
            expert_kernel,
            gu_parts=tuple((i, at, x.shape[0]) for i, at, x in gu),
            dn_parts=tuple((i, at, x.shape[0]) for i, at, x in dn),
        ),
        out_shape=jax.ShapeDtypeStruct((total, width), bf16),
        in_specs=[hbm] * (1 + len(gu) + len(dn)),
        out_specs=hbm,
        scratch_shapes=[
            pltpu.VMEM((total, width), bf16),
            pltpu.VMEM((parts, width, 2 * hid), bf16),
            pltpu.VMEM((parts * hid, width), bf16),
            pltpu.VMEM((total, parts * hid), bf16),
            pltpu.VMEM((total, width), bf16),
            pltpu.SemaphoreType.DMA((total // 256,)),
            pltpu.SemaphoreType.DMA((len(gu),)),
            pltpu.SemaphoreType.DMA((len(dn),)),
            pltpu.SemaphoreType.DMA((4,)),
        ],
        compiler_params=pltpu.CompilerParams(vmem_limit_bytes=48 * 2**20),
        cost_estimate=pl.CostEstimate(
            flops=6 * total * width * parts * hid, bytes_accessed=20 * 2**20, transcendentals=total * parts * hid
        ),
        name="expert_unit",
    )(rows, *[x for _, _, x in gu], *[x for _, _, x in dn])


def combine_kernel(rank, ids_ref, gates_ref, gain_ref, *rest, experts, split):
    backs = rest[: len(split)]
    out_ref, back_v, spread_v, acc_v, sem = rest[len(split) :]
    top, tokens = ids_ref.shape
    width = back_v.shape[1]
    chunks = sem.shape[1]
    cols = width // chunks
    copies = [[] for _ in range(chunks)]
    at = 0
    for j, back in enumerate(backs):
        size = back.shape[0]
        for c in range(chunks):
            span = pl.ds(c * cols, cols)
            copies[c].append(
                pltpu.make_async_copy(back.at[:, span], back_v.at[pl.ds(at, size), span], sem.at[j, c])
            )
        at += size
    for cs in copies:
        for c in cs:
            c.start()
    ids = ids_ref[...]
    gates = gates_ref[...]
    line = lax.broadcasted_iota(jnp.int32, (experts, tokens), 0)
    weight = jnp.zeros((experts, tokens), f32)
    for k in range(top):
        weight = weight + jnp.where(ids[k : k + 1, :] == line, gates[k : k + 1, :], 0.0)
    filler = jnp.zeros((tokens - 2 * experts, tokens), f32)
    table = jnp.transpose(jnp.concatenate([routing(ids, experts), weight, filler], axis=0))
    lanes = 128
    lane = lax.broadcasted_iota(jnp.int32, (tokens, lanes), 1)
    base, first = 0, 0
    for n in split:
        per = lanes // n
        owner = lane // n
        col = (lane % n + first).astype(f32)
        for e in range(0, experts, per):
            spread = jnp.zeros((tokens, lanes), f32)
            for q in range(per):
                hit = (owner == q) & (col == table[:, e + q : e + q + 1])
                spread = jnp.where(hit, table[:, experts + e + q : experts + e + q + 1], spread)
            for p in range(3):
                part = spread.astype(bf16)
                spread_v[p * tokens : (p + 1) * tokens, base : base + lanes] = part
                spread = spread - part.astype(f32)
            base += lanes
        first += n
    total_sq = jnp.zeros((tokens, 1), f32)
    for c in range(chunks):
        for copy in copies[c]:
            copy.wait()
        span = pl.ds(c * cols, cols)
        prod = jnp.dot(spread_v[...], back_v[:, span], preferred_element_type=f32)
        combined = prod[:tokens] + prod[tokens : 2 * tokens] + prod[2 * tokens :]
        total_sq = total_sq + jnp.sum(combined * combined, axis=-1, keepdims=True)
        acc_v[:, span] = combined
    scale = lax.rsqrt(total_sq / width + epsilon)
    slices, _, w = out_ref.shape
    for i in range(slices):
        span = pl.ds(i * w, w)
        out_ref[i] = (acc_v[:, span] * scale * gain_ref[:, span]).astype(bf16)


def combine(rank, ids, gates, gain, backs, rows, experts, split, slices):
    width = backs[0].shape[1]
    top = ids.shape[0]
    return pl.pallas_call(
        functools.partial(combine_kernel, experts=experts, split=split),
        out_shape=jax.ShapeDtypeStruct((slices, rows, width // slices), bf16),
        grid_spec=pltpu.PrefetchScalarGridSpec(
            num_scalar_prefetch=1,
            grid=(1,),
            in_specs=[
                pl.BlockSpec((top, rows), lambda s, r: (0, r[0])),
                pl.BlockSpec((top, rows), lambda s, r: (0, r[0])),
                pl.BlockSpec((1, width), lambda s, r: (0, 0)),
            ]
            + [pl.BlockSpec(memory_space=pl.ANY)] * len(split),
            out_specs=pl.BlockSpec((slices, rows, width // slices), lambda s, r: (0, 0, 0)),
            scratch_shapes=[
                pltpu.VMEM((experts * sum(split), width), bf16),
                pltpu.VMEM((3 * rows, experts * sum(split)), bf16),
                pltpu.VMEM((rows, width), f32),
                pltpu.SemaphoreType.DMA((len(split), 4)),
            ],
        ),
        name="combine",
    )(rank, ids, gates, gain, *backs)


def moved(x, step):
    n = lax.axis_size("tp")
    return lax.ppermute(x, "tp", [(i, step(i)) for i in range(n)])


def local(
    tokens, expert_ids, gate_values, norm_gain, gate_weight, up_weight, down_weight, out_gain
):
    experts = lax.axis_size("ep")
    n_tp = lax.axis_size("tp")
    rows, width = tokens.shape
    cap = rows // 2
    rank = lax.axis_index("tp").reshape(1).astype(jnp.int32)
    ids, gates = expert_ids.T, gate_values.T

    gu_own = jnp.concatenate([gate_weight[0], up_weight[0]], axis=1)
    dn_own = down_weight[0]

    def spread_out(x):
        up, down, other = (lambda i: (i + 2) % n_tp), (lambda i: (i - 2) % n_tp), (lambda i: i ^ 1)
        half = x.shape[0] // 2
        p = moved(x, up)
        m = moved(x, down)
        lo = moved(p[:half], up)
        hi = moved(m[half:], down)
        near = [(0, 0, x), (2, 0, p), (4, 0, m), (6, 0, lo), (6, half, hi)]
        far = [(i + 1, at, moved(a, other)) for i, at, a in near]
        return sorted(near + far, key=lambda entry: entry[:2])

    gu = spread_out(gu_own)
    dn = spread_out(dn_own)

    gain_full = lax.all_gather(out_gain, "tp", axis=0, tiled=True)
    split = SPLIT(cap)
    outgoing = dispatch(rank, tokens, ids, norm_gain.reshape(1, width), experts, split)
    backs = []
    for x in outgoing:
        arrived = lax.all_to_all(x, "ep", split_axis=0, concat_axis=0, tiled=True)
        result = expert_unit(arrived.reshape(-1, width), gu, dn, n_tp, down_weight.shape[1])
        back = lax.all_to_all(
            result.reshape(x.shape), "ep", split_axis=0, concat_axis=0, tiled=True
        )
        backs.append(back.reshape(-1, width))
    mixed = combine(
        rank, ids, gates, gain_full.reshape(1, width), backs, rows, experts, split, n_tp,
    )
    final = lax.all_to_all(mixed, "tp", split_axis=0, concat_axis=0, tiled=True)
    return final.reshape(n_tp * rows, width // n_tp)


def solution(mesh):
    in_specs = (
        P(("ep", "tp"), None),
        P("ep", None),
        P("ep", None),
        P(),
        P("ep", None, "tp"),
        P("ep", None, "tp"),
        P("ep", "tp", None),
        P("tp"),
    )
    out_specs = P("ep", "tp")
    return jax.shard_map(local, mesh=mesh, in_specs=in_specs, out_specs=out_specs, check_vma=False)
```

```python
import functools
import jax
import jax.numpy as jnp
from jax import lax
from jax.experimental import pallas as pl
from jax.experimental.pallas import tpu as pltpu
from jax.sharding import PartitionSpec as P

epsilon = 1e-05
clamp_limit = 7.0
sigmoid_alpha = 1.702
f32, bf16 = jnp.float32, jnp.bfloat16


def SPLIT(cap):
    return (cap,)


def routing(ids, experts):
    top, tokens = ids.shape
    line = lax.broadcasted_iota(jnp.int32, (experts, tokens), 0)
    named = jnp.zeros((experts, tokens), f32)
    for k in range(top):
        named = named + jnp.where(ids[k : k + 1, :] == line, 1.0, 0.0)
    row = lax.broadcasted_iota(jnp.int32, (tokens, tokens), 0)
    col = lax.broadcasted_iota(jnp.int32, (tokens, tokens), 1)
    before = jnp.where(row < col, 1.0, 0.0).astype(bf16)
    earlier = jnp.dot(named.astype(bf16), before, preferred_element_type=f32)
    return jnp.where(named > 0.5, earlier, -1000.0)


def dispatch_kernel(rank, tokens_ref, ids_ref, gain_ref, *rest, experts, cap):
    outs, (normed_ref, slot_ref) = rest[:-2], rest[-2:]
    tokens = tokens_ref.shape[0]
    group = outs[0].shape[0]

    @pl.when(pl.program_id(0) == 0)
    def _():
        values = tokens_ref[...].astype(f32)
        mean_sq = jnp.mean(values * values, axis=-1, keepdims=True)
        normed_ref[...] = (values * lax.rsqrt(mean_sq + epsilon) * gain_ref[...]).astype(bf16)
        slots = routing(ids_ref[...], experts)
        for i in range(experts // group):
            slot_ref[i] = slots[i * group : (i + 1) * group]

    slots = slot_ref[pl.program_id(0)]
    want = lax.broadcasted_iota(jnp.int32, (cap, tokens), 0).astype(f32)
    chosen = jnp.concatenate(
        [jnp.where(slots[i : i + 1] == want, 1.0, 0.0).astype(bf16) for i in range(group)], axis=0
    )
    picked = jnp.dot(chosen, normed_ref[...], preferred_element_type=f32).astype(bf16)
    for i in range(group):
        at = i * cap
        for out in outs:
            out[i] = picked[at : at + out.shape[1]]
            at += out.shape[1]


def dispatch(rank, tokens, ids, gain, experts, split):
    rows, width = tokens.shape
    group = 4
    return pl.pallas_call(
        functools.partial(dispatch_kernel, experts=experts, cap=sum(split)),
        out_shape=[jax.ShapeDtypeStruct((experts, n, width), bf16) for n in split],
        grid_spec=pltpu.PrefetchScalarGridSpec(
            num_scalar_prefetch=1,
            grid=(experts // group,),
            in_specs=[
                pl.BlockSpec((rows, width), lambda e, r: (0, 0)),
                pl.BlockSpec((ids.shape[0], rows), lambda e, r: (0, r[0])),
                pl.BlockSpec((1, width), lambda e, r: (0, 0)),
            ],
            out_specs=[pl.BlockSpec((group, n, width), lambda e, r: (e, 0, 0)) for n in split],
            scratch_shapes=[
                pltpu.VMEM((rows, width), bf16),
                pltpu.VMEM((experts // group, group, rows), f32),
            ],
        ),
        name="dispatch",
    )(rank, tokens, ids, gain)


def expert_kernel(rows_hbm, *rest, gu_parts, dn_parts):
    gu = rest[: len(gu_parts)]
    dn = rest[len(gu_parts) : len(gu_parts) + len(dn_parts)]
    out_hbm, rows_v, gu_v, dn_v, act_v, out_v, row_sem, gu_sem, dn_sem, out_sem = rest[len(gu_parts) + len(dn_parts) :]
    parts = gu_v.shape[0]
    hid = gu_v.shape[2] // 2
    total, width = rows_v.shape
    nrow = row_sem.shape[0]
    step = total // nrow
    nout = out_sem.shape[0]
    ocols = width // nout

    row_copies = [
        pltpu.make_async_copy(
            rows_hbm.at[pl.ds(i * step, step)], rows_v.at[pl.ds(i * step, step)], row_sem.at[i]
        )
        for i in range(nrow)
    ]
    gu_copies = [[] for _ in range(parts)]
    for j, (i, at, size) in enumerate(gu_parts):
        gu_copies[i].append(
            pltpu.make_async_copy(gu[j], gu_v.at[i, pl.ds(at, size)], gu_sem.at[j])
        )
    dn_copies = [[] for _ in range(parts)]
    for j, (i, at, size) in enumerate(dn_parts):
        dn_copies[i].append(
            pltpu.make_async_copy(dn[j], dn_v.at[pl.ds(i * hid + at, size)], dn_sem.at[j])
        )
    for c in gu_copies[0] + row_copies + gu_copies[1]:
        c.start()
    for i in range(parts):
        for c in (gu_copies[i + 2] if i + 2 < parts else []) + dn_copies[i]:
            c.start()
        for c in gu_copies[i]:
            c.wait()
        for m in range(nrow):
            if i == 0:
                row_copies[m].wait()
            span = pl.ds(m * step, step)
            h = jnp.dot(rows_v[span, :], gu_v[i], preferred_element_type=f32)
            g = jnp.minimum(h[:, :hid], clamp_limit)
            u = jnp.clip(h[:, hid:], -clamp_limit, clamp_limit)
            act = g * jax.nn.sigmoid(sigmoid_alpha * g) * (u + 1.0)
            act_v[span, i * hid : (i + 1) * hid] = act.astype(bf16)
    for cs in dn_copies:
        for c in cs:
            c.wait()
    out_copies = []
    for n in range(nout):
        cols = pl.ds(n * ocols, ocols)
        out_v[:, cols] = jnp.dot(act_v[...], dn_v[:, cols], preferred_element_type=f32).astype(bf16)
        c = pltpu.make_async_copy(out_v.at[:, cols], out_hbm.at[:, cols], out_sem.at[n])
        c.start()
        out_copies.append(c)
    for c in out_copies:
        c.wait()


def expert_unit(rows, gu, dn, parts, hid):
    total, width = rows.shape
    hbm = pl.BlockSpec(memory_space=pl.ANY)
    return pl.pallas_call(
        functools.partial(
            expert_kernel,
            gu_parts=tuple((i, at, x.shape[0]) for i, at, x in gu),
            dn_parts=tuple((i, at, x.shape[0]) for i, at, x in dn),
        ),
        out_shape=jax.ShapeDtypeStruct((total, width), bf16),
        in_specs=[hbm] * (1 + len(gu) + len(dn)),
        out_specs=hbm,
        scratch_shapes=[
            pltpu.VMEM((total, width), bf16),
            pltpu.VMEM((parts, width, 2 * hid), bf16),
            pltpu.VMEM((parts * hid, width), bf16),
            pltpu.VMEM((total, parts * hid), bf16),
            pltpu.VMEM((total, width), bf16),
            pltpu.SemaphoreType.DMA((total // 256,)),
            pltpu.SemaphoreType.DMA((len(gu),)),
            pltpu.SemaphoreType.DMA((len(dn),)),
            pltpu.SemaphoreType.DMA((4,)),
        ],
        compiler_params=pltpu.CompilerParams(vmem_limit_bytes=60 * 2**20),
        cost_estimate=pl.CostEstimate(
            flops=6 * total * width * parts * hid, bytes_accessed=20 * 2**20, transcendentals=total * parts * hid
        ),
        name="expert_unit",
    )(rows, *[x for _, _, x in gu], *[x for _, _, x in dn])


def combine_kernel(rank, ids_ref, gates_ref, gain_ref, *rest, experts, split):
    backs = rest[: len(split)]
    out_ref, back_v, spread_v, acc_v, sem = rest[len(split) :]
    top, tokens = ids_ref.shape
    width = back_v.shape[1]
    chunks = sem.shape[1]
    cols = width // chunks
    copies = [[] for _ in range(chunks)]
    at = 0
    for j, back in enumerate(backs):
        size = back.shape[0]
        for c in range(chunks):
            span = pl.ds(c * cols, cols)
            copies[c].append(
                pltpu.make_async_copy(back.at[:, span], back_v.at[pl.ds(at, size), span], sem.at[j, c])
            )
        at += size
    for cs in copies:
        for c in cs:
            c.start()
    ids = ids_ref[...]
    gates = gates_ref[...]
    line = lax.broadcasted_iota(jnp.int32, (experts, tokens), 0)
    weight = jnp.zeros((experts, tokens), f32)
    for k in range(top):
        weight = weight + jnp.where(ids[k : k + 1, :] == line, gates[k : k + 1, :], 0.0)
    filler = jnp.zeros((tokens - 2 * experts, tokens), f32)
    table = jnp.transpose(jnp.concatenate([routing(ids, experts), weight, filler], axis=0))
    lanes = 128
    lane = lax.broadcasted_iota(jnp.int32, (tokens, lanes), 1)
    base, first = 0, 0
    for n in split:
        per = lanes // n
        owner = lane // n
        col = (lane % n + first).astype(f32)
        for e in range(0, experts, per):
            spread = jnp.zeros((tokens, lanes), f32)
            for q in range(per):
                hit = (owner == q) & (col == table[:, e + q : e + q + 1])
                spread = jnp.where(hit, table[:, experts + e + q : experts + e + q + 1], spread)
            for p in range(2):
                part = spread.astype(bf16)
                spread_v[p * tokens : (p + 1) * tokens, base : base + lanes] = part
                spread = spread - part.astype(f32)
            base += lanes
        first += n
    total_sq = jnp.zeros((tokens, 1), f32)
    for c in range(chunks):
        for copy in copies[c]:
            copy.wait()
        span = pl.ds(c * cols, cols)
        prod = jnp.dot(spread_v[...], back_v[:, span], preferred_element_type=f32)
        combined = prod[:tokens] + prod[tokens:]
        total_sq = total_sq + jnp.sum(combined * combined, axis=-1, keepdims=True)
        acc_v[:, span] = combined
    scale = lax.rsqrt(total_sq / width + epsilon)
    slices, _, w = out_ref.shape
    for i in range(slices):
        span = pl.ds(i * w, w)
        out_ref[i] = (acc_v[:, span] * scale * gain_ref[:, span]).astype(bf16)


def combine(rank, ids, gates, gain, backs, rows, experts, split, slices):
    width = backs[0].shape[1]
    top = ids.shape[0]
    return pl.pallas_call(
        functools.partial(combine_kernel, experts=experts, split=split),
        out_shape=jax.ShapeDtypeStruct((slices, rows, width // slices), bf16),
        grid_spec=pltpu.PrefetchScalarGridSpec(
            num_scalar_prefetch=1,
            grid=(1,),
            in_specs=[
                pl.BlockSpec((top, rows), lambda s, r: (0, r[0])),
                pl.BlockSpec((top, rows), lambda s, r: (0, r[0])),
                pl.BlockSpec((1, width), lambda s, r: (0, 0)),
            ]
            + [pl.BlockSpec(memory_space=pl.ANY)] * len(split),
            out_specs=pl.BlockSpec((slices, rows, width // slices), lambda s, r: (0, 0, 0)),
            scratch_shapes=[
                pltpu.VMEM((experts * sum(split), width), bf16),
                pltpu.VMEM((2 * rows, experts * sum(split)), bf16),
                pltpu.VMEM((rows, width), f32),
                pltpu.SemaphoreType.DMA((len(split), 4)),
            ],
        ),
        name="combine",
    )(rank, ids, gates, gain, *backs)


def moved(x, step):
    n = lax.axis_size("tp")
    return lax.ppermute(x, "tp", [(i, step(i)) for i in range(n)])


def local(
    tokens, expert_ids, gate_values, norm_gain, gate_weight, up_weight, down_weight, out_gain
):
    experts = lax.axis_size("ep")
    n_tp = lax.axis_size("tp")
    rows, width = tokens.shape
    cap = rows // 2
    rank = lax.axis_index("tp").reshape(1).astype(jnp.int32)
    ids, gates = expert_ids.T, gate_values.T

    gu_own = jnp.concatenate([gate_weight[0], up_weight[0]], axis=1)
    dn_own = down_weight[0]

    def spread_out(x):
        up, down, other = (lambda i: (i + 2) % n_tp), (lambda i: (i - 2) % n_tp), (lambda i: i ^ 1)
        half = x.shape[0] // 2
        p = moved(x, up)
        m = moved(x, down)
        lo = moved(p[:half], up)
        hi = moved(m[half:], down)
        near = [(0, 0, x), (2, 0, p), (4, 0, m), (6, 0, lo), (6, half, hi)]
        far = [(i + 1, at, moved(a, other)) for i, at, a in near]
        return sorted(near + far, key=lambda entry: entry[:2])

    gu = spread_out(gu_own)
    dn = spread_out(dn_own)

    gain_full = lax.all_gather(out_gain, "tp", axis=0, tiled=True)
    split = SPLIT(cap)
    outgoing = dispatch(rank, tokens, ids, norm_gain.reshape(1, width), experts, split)
    backs = []
    for x in outgoing:
        arrived = lax.all_to_all(x, "ep", split_axis=0, concat_axis=0, tiled=True)
        result = expert_unit(arrived.reshape(-1, width), gu, dn, n_tp, down_weight.shape[1])
        back = lax.all_to_all(
            result.reshape(x.shape), "ep", split_axis=0, concat_axis=0, tiled=True
        )
        backs.append(back.reshape(-1, width))
    mixed = combine(
        rank, ids, gates, gain_full.reshape(1, width), backs, rows, experts, split, n_tp,
    )
    final = lax.all_to_all(mixed, "tp", split_axis=0, concat_axis=0, tiled=True)
    return final.reshape(n_tp * rows, width // n_tp)


def solution(mesh):
    in_specs = (
        P(("ep", "tp"), None),
        P("ep", None),
        P("ep", None),
        P(),
        P("ep", None, "tp"),
        P("ep", None, "tp"),
        P("ep", "tp", None),
        P("tp"),
    )
    out_specs = P("ep", "tp")
    return jax.shard_map(local, mesh=mesh, in_specs=in_specs, out_specs=out_specs, check_vma=False)
```

```python
import functools
import jax
import jax.numpy as jnp
from jax import lax
from jax.experimental import pallas as pl
from jax.experimental.pallas import tpu as pltpu
from jax.sharding import PartitionSpec as P

epsilon = 1e-05
clamp_limit = 7.0
sigmoid_alpha = 1.702
f32, bf16 = jnp.float32, jnp.bfloat16


def SPLIT(cap):
    return (cap,)


def routing(ids, experts):
    top, tokens = ids.shape
    line = lax.broadcasted_iota(jnp.int32, (experts, tokens), 0)
    named = jnp.zeros((experts, tokens), f32)
    for k in range(top):
        named = named + jnp.where(ids[k : k + 1, :] == line, 1.0, 0.0)
    row = lax.broadcasted_iota(jnp.int32, (tokens, tokens), 0)
    col = lax.broadcasted_iota(jnp.int32, (tokens, tokens), 1)
    before = jnp.where(row < col, 1.0, 0.0).astype(bf16)
    earlier = jnp.dot(named.astype(bf16), before, preferred_element_type=f32)
    return jnp.where(named > 0.5, earlier, -1000.0)


def dispatch_kernel(rank, tokens_ref, ids_ref, gain_ref, *rest, experts, cap):
    outs, (normed_ref, slot_ref) = rest[:-2], rest[-2:]
    tokens = tokens_ref.shape[0]
    group = outs[0].shape[0]

    @pl.when(pl.program_id(0) == 0)
    def _():
        values = tokens_ref[...].astype(f32)
        mean_sq = jnp.mean(values * values, axis=-1, keepdims=True)
        normed_ref[...] = (values * lax.rsqrt(mean_sq + epsilon) * gain_ref[...]).astype(bf16)
        slots = routing(ids_ref[...], experts)
        for i in range(experts // group):
            slot_ref[i] = slots[i * group : (i + 1) * group]

    slots = slot_ref[pl.program_id(0)]
    want = lax.broadcasted_iota(jnp.int32, (cap, tokens), 0).astype(f32)
    chosen = jnp.concatenate(
        [jnp.where(slots[i : i + 1] == want, 1.0, 0.0).astype(bf16) for i in range(group)], axis=0
    )
    picked = jnp.dot(chosen, normed_ref[...], preferred_element_type=f32).astype(bf16)
    for i in range(group):
        at = i * cap
        for out in outs:
            out[i] = picked[at : at + out.shape[1]]
            at += out.shape[1]


def dispatch(rank, tokens, ids, gain, experts, split):
    rows, width = tokens.shape
    group = 4
    return pl.pallas_call(
        functools.partial(dispatch_kernel, experts=experts, cap=sum(split)),
        out_shape=[jax.ShapeDtypeStruct((experts, n, width), bf16) for n in split],
        grid_spec=pltpu.PrefetchScalarGridSpec(
            num_scalar_prefetch=1,
            grid=(experts // group,),
            in_specs=[
                pl.BlockSpec((rows, width), lambda e, r: (0, 0)),
                pl.BlockSpec((ids.shape[0], rows), lambda e, r: (0, r[0])),
                pl.BlockSpec((1, width), lambda e, r: (0, 0)),
            ],
            out_specs=[pl.BlockSpec((group, n, width), lambda e, r: (e, 0, 0)) for n in split],
            scratch_shapes=[
                pltpu.VMEM((rows, width), bf16),
                pltpu.VMEM((experts // group, group, rows), f32),
            ],
        ),
        name="dispatch",
    )(rank, tokens, ids, gain)


def expert_kernel(rows_hbm, early_hbm, *rest, gu_parts, dn_parts):
    gu = rest[: len(gu_parts)]
    dn = rest[len(gu_parts) : len(gu_parts) + len(dn_parts)]
    out_hbm, rows_v, gu_v, dn_v, act_v, out_v, row_sem, gu_sem, dn_sem, out_sem = rest[len(gu_parts) + len(dn_parts) :]
    parts = gu_v.shape[0]
    hid = gu_v.shape[2] // 2
    total, width = rows_v.shape
    nrow = row_sem.shape[0]
    step = total // nrow
    nout = out_sem.shape[0]
    ocols = width // nout

    row_copies = [
        pltpu.make_async_copy(
            rows_hbm.at[pl.ds(i * step, step)], rows_v.at[pl.ds(i * step, step)], row_sem.at[i]
        )
        for i in range(nrow)
    ]
    gu_copies = [[] for _ in range(parts)]
    for j, (i, at, size) in enumerate(gu_parts):
        gu_copies[i].append(
            pltpu.make_async_copy(gu[j], gu_v.at[i, pl.ds(at, size)], gu_sem.at[j])
        )
    dn_copies = [[] for _ in range(parts)]
    for j, (i, at, size) in enumerate(dn_parts):
        dn_copies[i].append(
            pltpu.make_async_copy(dn[j], dn_v.at[pl.ds(i * hid + at, size)], dn_sem.at[j])
        )
    for c in gu_copies[0] + row_copies + gu_copies[1]:
        c.start()
    for i in range(parts):
        for c in (gu_copies[i + 2] if i + 2 < parts else []) + dn_copies[i]:
            c.start()
        for c in gu_copies[i]:
            c.wait()
        for m in range(nrow):
            if i == 0:
                row_copies[m].wait()
            span = pl.ds(m * step, step)
            h = jnp.dot(rows_v[span, :], gu_v[i], preferred_element_type=f32)
            g = jnp.minimum(h[:, :hid], clamp_limit)
            u = jnp.clip(h[:, hid:], -clamp_limit, clamp_limit)
            act = g * jax.nn.sigmoid(sigmoid_alpha * g) * (u + 1.0)
            act_v[span, i * hid : (i + 1) * hid] = act.astype(bf16)
    for cs in dn_copies:
        for c in cs:
            c.wait()
    out_copies = []
    for n in range(nout):
        cols = pl.ds(n * ocols, ocols)
        out_v[:, cols] = jnp.dot(act_v[...], dn_v[:, cols], preferred_element_type=f32).astype(bf16)
        c = pltpu.make_async_copy(out_v.at[:, cols], out_hbm.at[:, cols], out_sem.at[n])
        c.start()
        out_copies.append(c)
    for c in out_copies:
        c.wait()


def expert_unit(rows, early, gu, dn, parts, hid):
    total, width = rows.shape
    hbm = pl.BlockSpec(memory_space=pl.ANY)
    return pl.pallas_call(
        functools.partial(
            expert_kernel,
            gu_parts=tuple((i, at, x.shape[0]) for i, at, x in gu),
            dn_parts=tuple((i, at, x.shape[0]) for i, at, x in dn),
        ),
        out_shape=jax.ShapeDtypeStruct((total, width), bf16),
        in_specs=[hbm] * (2 + len(gu) + len(dn)),
        out_specs=hbm,
        scratch_shapes=[
            pltpu.VMEM((total, width), bf16),
            pltpu.VMEM((parts, width, 2 * hid), bf16),
            pltpu.VMEM((parts * hid, width), bf16),
            pltpu.VMEM((total, parts * hid), bf16),
            pltpu.VMEM((total, width), bf16),
            pltpu.SemaphoreType.DMA((total // 256,)),
            pltpu.SemaphoreType.DMA((len(gu),)),
            pltpu.SemaphoreType.DMA((len(dn),)),
            pltpu.SemaphoreType.DMA((4,)),
        ],
        compiler_params=pltpu.CompilerParams(vmem_limit_bytes=60 * 2**20),
        cost_estimate=pl.CostEstimate(
            flops=6 * total * width * parts * hid, bytes_accessed=20 * 2**20, transcendentals=total * parts * hid
        ),
        name="expert_unit",
    )(rows, early, *[x for _, _, x in gu], *[x for _, _, x in dn])


def combine_kernel(rank, ids_ref, gates_ref, gain_ref, *rest, experts, split):
    backs = rest[: len(split)]
    out_ref, back_v, spread_v, acc_v, sem = rest[len(split) :]
    top, tokens = ids_ref.shape
    width = back_v.shape[1]
    chunks = sem.shape[1]
    cols = width // chunks
    copies = [[] for _ in range(chunks)]
    at = 0
    for j, back in enumerate(backs):
        size = back.shape[0]
        for c in range(chunks):
            span = pl.ds(c * cols, cols)
            copies[c].append(
                pltpu.make_async_copy(back.at[:, span], back_v.at[pl.ds(at, size), span], sem.at[j, c])
            )
        at += size
    for cs in copies:
        for c in cs:
            c.start()
    ids = ids_ref[...]
    gates = gates_ref[...]
    line = lax.broadcasted_iota(jnp.int32, (experts, tokens), 0)
    weight = jnp.zeros((experts, tokens), f32)
    for k in range(top):
        weight = weight + jnp.where(ids[k : k + 1, :] == line, gates[k : k + 1, :], 0.0)
    filler = jnp.zeros((tokens - 2 * experts, tokens), f32)
    table = jnp.transpose(jnp.concatenate([routing(ids, experts), weight, filler], axis=0))
    lanes = 128
    lane = lax.broadcasted_iota(jnp.int32, (tokens, lanes), 1)
    base, first = 0, 0
    for n in split:
        per = lanes // n
        owner = lane // n
        col = (lane % n + first).astype(f32)
        for e in range(0, experts, per):
            spread = jnp.zeros((tokens, lanes), f32)
            for q in range(per):
                hit = (owner == q) & (col == table[:, e + q : e + q + 1])
                spread = jnp.where(hit, table[:, experts + e + q : experts + e + q + 1], spread)
            for p in range(2):
                part = spread.astype(bf16)
                spread_v[p * tokens : (p + 1) * tokens, base : base + lanes] = part
                spread = spread - part.astype(f32)
            base += lanes
        first += n
    total_sq = jnp.zeros((tokens, 1), f32)
    for c in range(chunks):
        for copy in copies[c]:
            copy.wait()
        span = pl.ds(c * cols, cols)
        prod = jnp.dot(spread_v[...], back_v[:, span], preferred_element_type=f32)
        combined = prod[:tokens] + prod[tokens:]
        total_sq = total_sq + jnp.sum(combined * combined, axis=-1, keepdims=True)
        acc_v[:, span] = combined
    scale = lax.rsqrt(total_sq / width + epsilon)
    slices, _, w = out_ref.shape
    for i in range(slices):
        span = pl.ds(i * w, w)
        gain = gain_ref[pl.ds(rank[0] ^ i, 1), :]
        out_ref[i] = (acc_v[:, span] * scale * gain).astype(bf16)


def combine(rank, ids, gates, gain, backs, rows, experts, split, slices):
    width = backs[0].shape[1]
    top = ids.shape[0]
    return pl.pallas_call(
        functools.partial(combine_kernel, experts=experts, split=split),
        out_shape=jax.ShapeDtypeStruct((slices, rows, width // slices), bf16),
        grid_spec=pltpu.PrefetchScalarGridSpec(
            num_scalar_prefetch=1,
            grid=(1,),
            in_specs=[
                pl.BlockSpec((top, rows), lambda s, r: (0, r[0])),
                pl.BlockSpec((top, rows), lambda s, r: (0, r[0])),
                pl.BlockSpec(gain.shape, lambda s, r: (0, 0)),
            ]
            + [pl.BlockSpec(memory_space=pl.ANY)] * len(split),
            out_specs=pl.BlockSpec((slices, rows, width // slices), lambda s, r: (0, 0, 0)),
            scratch_shapes=[
                pltpu.VMEM((experts * sum(split), width), bf16),
                pltpu.VMEM((2 * rows, experts * sum(split)), bf16),
                pltpu.VMEM((rows, width), f32),
                pltpu.SemaphoreType.DMA((len(split), 4)),
            ],
        ),
        name="combine",
    )(rank, ids, gates, gain, *backs)


def moved(x, step):
    n = lax.axis_size("tp")
    return lax.ppermute(x, "tp", [(i, step(i)) for i in range(n)])


def local(
    tokens, expert_ids, gate_values, norm_gain, gate_weight, up_weight, down_weight, out_gain
):
    experts = lax.axis_size("ep")
    n_tp = lax.axis_size("tp")
    rows, width = tokens.shape
    cap = rows // 2
    rank = lax.axis_index("tp").reshape(1).astype(jnp.int32)
    ids, gates = expert_ids.T, gate_values.T

    gu_own = jnp.concatenate([gate_weight[0], up_weight[0]], axis=1)
    dn_own = down_weight[0]

    def spread_out(x):
        up, down, other = (lambda i: (i + 2) % n_tp), (lambda i: (i - 2) % n_tp), (lambda i: i ^ 1)
        half = x.shape[0] // 2
        p = moved(x, up)
        m = moved(x, down)
        lo = moved(p[:half], up)
        hi = moved(m[half:], down)
        near = [(0, 0, x), (2, 0, p), (4, 0, m), (6, 0, lo), (6, half, hi)]
        far = [(i + 1, at, moved(a, other)) for i, at, a in near]
        return sorted(near + far, key=lambda entry: entry[:2])

    gu = spread_out(gu_own)
    dn = spread_out(dn_own)

    gains = [out_gain.reshape(1, -1)]
    for d in range(1, n_tp):
        gains.append(moved(gains[0], lambda i: i ^ d))
    gain_near = jnp.concatenate(gains, axis=0)
    split = SPLIT(cap)
    outgoing = dispatch(rank, tokens, ids, norm_gain.reshape(1, width), experts, split)
    backs = []
    for x in outgoing:
        arrived = lax.all_to_all(x, "ep", split_axis=0, concat_axis=0, tiled=True)
        result = expert_unit(arrived.reshape(-1, width), gain_near, gu, dn, n_tp, down_weight.shape[1])
        back = lax.all_to_all(
            result.reshape(x.shape), "ep", split_axis=0, concat_axis=0, tiled=True
        )
        backs.append(back.reshape(-1, width))
    mixed = combine(
        rank, ids, gates, gain_near, backs, rows, experts, split, n_tp,
    )
    final = lax.all_to_all(mixed, "tp", split_axis=0, concat_axis=0, tiled=True)
    return final.reshape(n_tp * rows, width // n_tp)


def solution(mesh):
    in_specs = (
        P(("ep", "tp"), None),
        P("ep", None),
        P("ep", None),
        P(),
        P("ep", None, "tp"),
        P("ep", None, "tp"),
        P("ep", "tp", None),
        P("tp"),
    )
    out_specs = P("ep", "tp")
    return jax.shard_map(local, mesh=mesh, in_specs=in_specs, out_specs=out_specs, check_vma=False)
```
